512 devices in a mesh: sp: 32 (over z, x), tp: 16 (over y, core).
Axes of the slice: x: 4, y: 8, z: 8, core: 2. Of those that a mesh axis runs over, the one named last changes fastest.
Arguments:
- residual_in: bfloat16 [6144, 2048], P('sp', 'tp'), may hold values from -6 to 6
- query_rows: bfloat16 [6144, 1024], P('sp', 'tp'), may hold values from -8 to 8
- key_rows: bfloat16 [6144, 1024], P('sp', 'tp'), may hold values from -8 to 8
- value_rows: bfloat16 [6144, 1024], P('sp', 'tp'), may hold values from -6 to 6
- map_weight: float32 [16], P('tp'), may hold values from 0.3 to 0.8
- head_gain: float32 [64], replicated, may hold values from 0.1 to 1.9
- out_proj: bfloat16 [1024, 2048], P(None, 'tp'), may hold values from -0.1875 to 0.1875
- norm_gain: float32 [2048], replicated, may hold values from 0.1 to 1.9
- route_ids: int32 [6144, 2], P('sp'), may hold values from 0 to 31, all different within a row; in each aligned block of 192 rows (0 to 191, 192 to 383, ...) at most 15 rows name the same one
- route_weights: float32 [6144, 2], P('sp'), may hold values from 0.2 to 1.2
- expert_gate: bfloat16 [32, 1024, 2048], P('sp', 'tp'), may hold values from -0.125 to 0.125
- expert_up: bfloat16 [32, 1024, 2048], P('sp', 'tp'), may hold values from -0.125 to 0.125
- expert_down: bfloat16 [32, 1024, 2048], P('sp', None, 'tp'), may hold values from -0.1875 to 0.1875
- shared_gate: bfloat16 [1024, 2048], P('tp'), may hold values from -0.125 to 0.125
- shared_up: bfloat16 [1024, 2048], P('tp'), may hold values from -0.125 to 0.125
- shared_down: bfloat16 [1024, 2048], P(None, 'tp'), may hold values from -0.1875 to 0.1875
Outputs:
- mixed_out: bfloat16 [6144, 2048], P('sp', 'tp')
The draws below stay inside these ranges and needn't reach their ends.
Inputs may be any that keep to these rules, and one draw needn't show every extreme that they name: `route_ids`: each row names 2 different experts. Among the rows held by one index of sp no expert is named more than 15 times, and in every draw some expert is named exactly 15 times by the rows of some index of sp.
All inputs are finite; a program needn't handle non-finite values.
Results may differ from the reference program's by a relative error of at most 0.0095.
Values may be sent and summed in bfloat16 or wider, within the bound.
A program may use at most 64 MiB of HBM per device.

```python
import math
from functools import partial
import jax
import jax.numpy as jnp
import numpy as np
from jax import lax

D = 2048
H = 16
HD = 64
FE = 1024
TOPK = 2
SEQ_DEV = 192
TOKENS = 6144
EXPERTS = 32
CAPACITY = 15
N_SP = 32


def query_key_pair(key):
    query_key = jax.random.fold_in(key, 11)
    second_key = jax.random.fold_in(key, 12)
    full_shape = (TOKENS, H * HD)
    queries = jnp.clip(jax.random.normal(query_key, full_shape, jnp.float32) * 1.3, -8.0, 8.0)
    key_vals = jnp.clip(jax.random.normal(second_key, full_shape, jnp.float32) * 1.3, -8.0, 8.0)
    return (queries, key_vals)


def draw_query_rows(key, part):
    return query_key_pair(key)[0].astype(jnp.bfloat16)


def draw_key_rows(key, part):
    return query_key_pair(key)[1].astype(jnp.bfloat16)


def block_scale(rng, extent, pieces, low, high):
    def one(dim, shards_of):
        heights = jax.random.uniform(jax.random.fold_in(jax.random.fold_in(rng, 6), dim), (shards_of,), jnp.float32, low / len(pieces), high / len(pieces))
        return jnp.repeat(jnp.exp(heights), extent[dim] // shards_of).reshape((-1,) + (1,) * (len(extent) - dim - 1))

    loudness = one(*pieces[0])
    for cut in pieces[1:]:
        loudness = loudness * one(*cut)
    return loudness


def deal_out(rng, own, number, rows, number_of, top, reach, slope):
    ranking = jax.random.permutation(rng, number_of)
    packed, usual = shares(number_of, rows * top, reach, slope, True), shares(number_of, rows * top, reach, slope, False)
    places = jnp.arange(number_of)

    def named(lengths, rotation):
        used = int((lengths > 0).sum())
        fixed = max(1, used // 4)
        passed = fixed + (places - fixed + rotation * (used - fixed)) % max(1, number_of - fixed)
        return jnp.zeros((number_of,), jnp.int32).at[ranking[jnp.where(places < fixed, places, passed)]].set(jnp.asarray(lengths, jnp.int32))

    lengths = jnp.where(number % 4 == 0, named(packed, number // 4), named(usual, number - number // 4 - 1))
    mixed = jax.random.permutation(jax.random.fold_in(own, 3), number_of)
    donor, receiver = mixed[0:number_of // 2 * 2:2], mixed[1:number_of // 2 * 2:2]
    slack = jnp.minimum(lengths[donor] - 1, reach - lengths[receiver]) // 2
    slack = jnp.where((donor == ranking[0]) | (receiver == ranking[0]) | (lengths[receiver] == 0), 0, jnp.maximum(slack, 0))
    passed = jax.random.randint(jax.random.fold_in(own, 4), (number_of // 2,), 0, 1 << 20) % (slack + 1)
    lengths = lengths.at[donor].add(-passed).at[receiver].add(passed)
    items = jnp.searchsorted(jnp.cumsum(lengths), jnp.arange(rows * top), side="right").astype(jnp.int32)
    listing = items.reshape(top, rows).T
    listing = listing[jax.random.permutation(jax.random.fold_in(own, 1), rows)]
    rotation = jax.random.randint(jax.random.fold_in(own, 2), (rows, 1), 0, top)
    return jnp.take_along_axis(listing, (jnp.arange(top)[None, :] + rotation) % top, axis=1)


def shares(amount, total, most, skew, full):
    loads = [(1 << 20) // math.isqrt(grade ** skew) + 1 for grade in range(1, amount + 1)]
    largest = most if full else min(most, max(-(-total // amount), total * loads[0] // sum(loads)))
    least = 1 if total - largest >= amount - 1 else 0
    given, rest = [largest] + [least] * (amount - 1), total - largest - least * (amount - 1)
    while rest > 0:
        movable = [i for i in range(1, amount) if given[i] < largest] or [i for i in range(1, amount) if given[i] < most]
        mass, remaining = sum([loads[i] for i in movable]), rest
        for i in movable:
            extra = min(most - given[i], max(1, remaining * loads[i] // mass), rest)
            given[i] = given[i] + extra
            rest = rest - extra
    return np.array(given)


def gaussian(rng, extent, spread, reach, cuts=(), kind=jnp.bfloat16):
    entries = spread * jax.random.normal(rng, extent, jnp.float32)
    if cuts:
        entries = entries * block_scale(rng, extent, cuts, -0.22, 0.18)
    return jnp.clip(entries, -reach, reach).astype(kind)


def setup_inputs(seed: int = 0) -> dict:
    seeds = jax.random.split(jax.random.key(seed), 17)
    residual_in = gaussian(seeds[0], (TOKENS, D), 1.0, 6.0, ((0, 32), (1, 16)))
    query_rows = draw_query_rows(jax.random.fold_in(seeds[16], 71), 0)
    key_rows = draw_key_rows(jax.random.fold_in(seeds[16], 71), 0)
    value_rows = gaussian(seeds[3], (TOKENS, H * HD), 1.0, 6.0, ((0, 32), (1, 16)))
    map_weight = jnp.clip(0.3 + 0.5 * jax.random.uniform(seeds[4], (H,), jnp.float32) ** block_scale(seeds[4], (H,), ((0, 16),), -0.2, 0.2), 0.3, 0.8)
    head_gain = jnp.clip(1.0 + 0.18 * jax.random.normal(seeds[5], (HD,), jnp.float32), 0.1, 1.9)
    out_proj = gaussian(seeds[6], (H * HD, D), (H * HD) ** -0.5, 0.1875, ((1, 16),))
    norm_gain = jnp.clip(1.0 + 0.18 * jax.random.normal(seeds[7], (D,), jnp.float32), 0.1, 1.9)
    route_ids_keys = jax.random.split(jax.random.fold_in(seeds[8], 1), TOKENS // SEQ_DEV)
    route_ids_turns = jax.random.permutation(jax.random.fold_in(seeds[8], 3), TOKENS // SEQ_DEV)
    route_ids = jax.vmap(lambda own, number: deal_out(jax.random.fold_in(seeds[8], 2), own, number, SEQ_DEV, EXPERTS, TOPK, CAPACITY, 2))(route_ids_keys, route_ids_turns).reshape((TOKENS, TOPK))
    route_weights = jnp.clip(0.2 + 1 * jax.random.uniform(seeds[9], (TOKENS, TOPK), jnp.float32) ** block_scale(seeds[9], (TOKENS, TOPK), ((0, 32),), -0.2, 0.2), 0.2, 1.2)
    expert_gate = gaussian(seeds[10], (EXPERTS, FE, D), D ** -0.5, 0.125, ((0, 32), (1, 16)))
    expert_up = gaussian(seeds[11], (EXPERTS, FE, D), D ** -0.5, 0.125, ((0, 32), (1, 16)))
    expert_down = gaussian(seeds[12], (EXPERTS, FE, D), FE ** -0.5, 0.1875, ((0, 32), (2, 16)))
    shared_gate = gaussian(seeds[13], (FE, D), D ** -0.5, 0.125, ((0, 16),))
    shared_up = gaussian(seeds[14], (FE, D), D ** -0.5, 0.125, ((0, 16),))
    shared_down = gaussian(seeds[15], (FE, D), FE ** -0.5, 0.1875, ((1, 16),))
    return {"residual_in": residual_in, "query_rows": query_rows, "key_rows": key_rows, "value_rows": value_rows, "map_weight": map_weight, "head_gain": head_gain, "out_proj": out_proj, "norm_gain": norm_gain, "route_ids": route_ids, "route_weights": route_weights, "expert_gate": expert_gate, "expert_up": expert_up, "expert_down": expert_down, "shared_gate": shared_gate, "shared_up": shared_up, "shared_down": shared_down}


epsilon = 1e-06
masked_score = -1e+30

def rms_scale(values, gain_vec):
    squares = lax.optimization_barrier(jnp.mean(values * values, axis=-1, keepdims=True))
    return values * lax.rsqrt(squares + epsilon) * gain_vec

def block_slots(route_block, experts_all, capacity):
    flat_ids = route_block.reshape(-1)
    one_hot = (flat_ids[:, None] == jnp.arange(experts_all, dtype=jnp.int32)[None, :]).astype(jnp.int32)
    earlier = jnp.cumsum(one_hot, axis=0) - one_hot
    position = lax.optimization_barrier(jnp.sum(earlier * one_hot, axis=1))
    return (flat_ids * capacity + position).astype(jnp.int32).reshape(route_block.shape)

def reference(residual_in, query_rows, key_rows, value_rows, map_weight, head_gain, out_proj, norm_gain, route_ids, route_weights, expert_gate, expert_up, expert_down, shared_gate, shared_up, shared_down):
    half_dim = HD // 2
    block_len = min(256, TOKENS)
    block_count = TOKENS // block_len
    key_heads = key_rows.reshape(TOKENS, H, 2, half_dim).astype(jnp.float32)
    value_heads = value_rows.reshape(TOKENS, H, HD).astype(jnp.float32)
    query_blocks = query_rows.reshape(block_count, block_len, H, 2, half_dim)
    key_pos = jnp.arange(TOKENS, dtype=jnp.int32)

    def attend(operands):
        query_block, block_index = operands
        query_pos = block_index * block_len + jnp.arange(block_len, dtype=jnp.int32)
        scores = jnp.einsum('qhmd,khmd->mhqk', query_block.astype(jnp.float32), key_heads) * half_dim ** (-0.5)
        visible = key_pos[None, :] <= query_pos[:, None]
        scores = jnp.where(visible, scores, masked_score)
        row_max = lax.optimization_barrier(jnp.max(scores, axis=-1, keepdims=True))
        expo = jnp.where(visible, jnp.exp(scores - row_max), 0.0)
        totals = lax.optimization_barrier(jnp.sum(expo, axis=-1))
        rounded = lax.optimization_barrier(expo.astype(jnp.bfloat16)).astype(jnp.float32)
        summed = jnp.einsum('mhqk,khd->mhqd', rounded, value_heads) / totals[..., None]
        return summed[0] - map_weight[:, None, None] * summed[1]
    parts = lax.map(attend, (query_blocks, jnp.arange(block_count, dtype=jnp.int32)))
    head_out = rms_scale(parts, head_gain).astype(jnp.bfloat16)
    head_out = jnp.transpose(head_out, (0, 2, 1, 3)).reshape(TOKENS, H * HD)
    attn = jnp.dot(head_out, out_proj, preferred_element_type=jnp.float32)
    hidden_state = (residual_in.astype(jnp.float32) + attn).astype(jnp.bfloat16)
    normed = rms_scale(hidden_state.astype(jnp.float32), norm_gain).astype(jnp.bfloat16)
    shared_hidden = (jax.nn.silu(jnp.dot(normed, shared_gate.T, preferred_element_type=jnp.float32)) * jnp.dot(normed, shared_up.T, preferred_element_type=jnp.float32)).astype(jnp.bfloat16)
    shared_out = jnp.dot(shared_hidden, shared_down, preferred_element_type=jnp.float32)
    slot_ids = jax.vmap(partial(block_slots, experts_all=EXPERTS, capacity=CAPACITY))(route_ids.reshape(N_SP, SEQ_DEV, TOPK))
    group_ids = jnp.broadcast_to(jnp.arange(N_SP, dtype=jnp.int32)[:, None, None], slot_ids.shape)
    token_ids = group_ids * SEQ_DEV + jnp.broadcast_to(jnp.arange(SEQ_DEV, dtype=jnp.int32)[None, :, None], slot_ids.shape)
    table = jnp.full((N_SP, EXPERTS * CAPACITY), TOKENS, jnp.int32).at[group_ids, slot_ids].set(token_ids)
    table = jnp.transpose(table.reshape(N_SP, EXPERTS, CAPACITY), (1, 0, 2))
    padded = jnp.concatenate([normed, jnp.zeros((1, D), jnp.bfloat16)], axis=0)

    def run_expert(operands):
        gate_w, up_w, down_w, rows_index = operands
        gathered = padded[rows_index.reshape(-1)]
        hidden_part = (jax.nn.silu(jnp.dot(gathered, gate_w.T, preferred_element_type=jnp.float32)) * jnp.dot(gathered, up_w.T, preferred_element_type=jnp.float32)).astype(jnp.bfloat16)
        return jnp.dot(hidden_part, down_w, preferred_element_type=jnp.float32).astype(jnp.bfloat16)
    results = lax.map(run_expert, (expert_gate, expert_up, expert_down, table))
    results = results.reshape(EXPERTS * N_SP * CAPACITY, D)
    expert_of = slot_ids // CAPACITY
    position = slot_ids % CAPACITY
    flat_index = ((expert_of * N_SP + group_ids) * CAPACITY + position).astype(jnp.int32).reshape(TOKENS, TOPK)
    picked = results[flat_index].astype(jnp.float32)
    routed = lax.optimization_barrier(jnp.sum(picked * route_weights[:, :, None], axis=1))
    return (hidden_state.astype(jnp.float32) + shared_out + routed).astype(jnp.bfloat16)
```

```python
import jax
import jax.numpy as jnp
from jax import lax
from jax.experimental import pallas as pl
from jax.experimental.pallas import tpu as pltpu
from jax.sharding import PartitionSpec as P

MESH = pl.DeviceIdType.MESH
EPS = 1e-06
MASKED = -1e30
NX, NZ, NY, NT = 4, 8, 8, 16
NSP = NX * NZ
S = 192
HS = S // 2
SLOT = 16
ROWS = NSP * SLOT
D = 2048
CW = 128
LOG2E = 1.4426950408889634
BF = jnp.bfloat16
F32 = jnp.float32
CP = 2
EP = 4
FP = 2


def kernel(
    res_ref, q_ref, k_ref, v_ref, mw_ref, hg_ref, ng_ref, ids_ref, rw_ref,
    wo_hbm, eg_hbm, eu_hbm, ed_hbm, sg_hbm, su_hbm, sd_hbm,
    out_ref,
    kvall, qbig, m_s, l_s, acc, wo, wgu, wd, sgu, sd, m0, m1,
    hb, hfull, hid, hidall, normed, sb, outg, eb, fb, hidx, res_o, ret,
    wsem, asend, zup, zdn, xsem, bsend, bring, bpair, csend, cup, cdn, cpair,
    ssend, sring, spair, dsend, drecv, esend, eup, edn, epair,
    fsend, fup, fdn, fpair, gsend, grecv,
):
    sp = lax.axis_index("sp")
    tp = lax.axis_index("tp")
    z, x = sp // NX, sp % NX
    y, c = tp // 2, tp % 2
    pair_dev = (sp, y * 2 + (1 - c))

    def zdev(step):
        return ((z + step + NZ) % NZ * NX + x, tp)

    def xdev(step):
        return (z * NX + (x + step + NX) % NX, tp)

    def ydev(step):
        return (sp, (y + step + NY) % NY * 2 + c)

    def rcopy(src, dst, ssem, rsem, dev):
        return pltpu.make_async_remote_copy(
            src_ref=src, dst_ref=dst, send_sem=ssem, recv_sem=rsem,
            device_id=dev, device_id_type=MESH,
        )

    def wait_bytes(view, sem):
        pltpu.make_async_copy(view, view, sem).wait()

    loads = [
        pltpu.make_async_copy(wo_hbm, wo, wsem.at[0]),
        pltpu.make_async_copy(eg_hbm.at[0], wgu.at[0:64], wsem.at[1]),
        pltpu.make_async_copy(eu_hbm.at[0], wgu.at[64:128], wsem.at[2]),
        pltpu.make_async_copy(ed_hbm.at[0], wd, wsem.at[3]),
        pltpu.make_async_copy(sg_hbm, sgu.at[0:64], wsem.at[4]),
        pltpu.make_async_copy(su_hbm, sgu.at[64:128], wsem.at[5]),
        pltpu.make_async_copy(sd_hbm, sd, wsem.at[6]),
    ]
    for load in loads:
        load.start()

    barrier = pltpu.get_barrier_semaphore()

    def greet_sp(i, carry):
        pl.semaphore_signal(barrier, inc=1, device_id=((sp + i) % NSP, tp), device_id_type=MESH)
        return carry

    def greet_tp(i, carry):
        pl.semaphore_signal(barrier, inc=1, device_id=(sp, (tp + i) % NT), device_id_type=MESH)
        return carry

    lax.fori_loop(1, NSP, greet_sp, 0)
    lax.fori_loop(1, NT, greet_tp, 0)

    kvall[sp] = jnp.concatenate([k_ref[...], v_ref[...]], axis=1)
    q = q_ref[...]
    lane64 = lax.broadcasted_iota(jnp.int32, (S, 64), 1)
    zero64 = jnp.zeros((S, 64), BF)
    q1 = jnp.where(lane64 < 32, q, zero64)
    q2 = jnp.where(lane64 >= 32, q, zero64)
    qbig[0:S, :] = jnp.concatenate([q1, zero64], axis=1)
    qbig[S:, :] = jnp.concatenate([q2, zero64], axis=1)
    m_s[...] = jnp.full((2 * S, CW), MASKED, F32)
    l_s[...] = jnp.zeros((2 * S, CW), F32)
    acc[...] = jnp.zeros((2 * S, CW), F32)

    pl.semaphore_wait(barrier, NSP - 1 + NT - 1)

    def slot(step, xs=0):
        return (z + step + NZ) % NZ * NX + (x + xs + NX) % NX

    def z_up(k):
        r = kvall.at[slot(-k)]
        return rcopy(r, r, asend.at[0], zup.at[k], zdev(1))

    def z_dn(k):
        r = kvall.at[slot(k)]
        return rcopy(r, r, asend.at[0], zdn.at[k], zdev(-1))

    steps = [0]
    for k in range(4):
        steps.append(-1 - k)
        if k < 3:
            steps.append(1 + k)

    def x_right(n):
        r = kvall.at[slot(steps[n])]
        return rcopy(r, r, asend.at[0], xsem.at[n, 0], xdev(1))

    def x_left(n):
        r = kvall.at[slot(steps[n])]
        return rcopy(r, r, asend.at[0], xsem.at[n, 1], xdev(-1))

    def relay_right(n):
        r = kvall.at[slot(steps[n], -1), 0:HS]
        return rcopy(r, r, asend.at[0], xsem.at[n, 2], xdev(1))

    def relay_left(n):
        r = kvall.at[slot(steps[n], 1), HS:S]
        return rcopy(r, r, asend.at[0], xsem.at[n, 3], xdev(-1))

    def x_send(n):
        x_right(n).start()
        x_left(n).start()

    def x_relay(n):
        x_right(n).wait_recv()
        relay_right(n).start()
        x_left(n).wait_recv()
        relay_left(n).start()

    def x_finish(n):
        relay_right(n).wait_recv()
        relay_left(n).wait_recv()

    scale2 = LOG2E * 32.0 ** (-0.5)

    def attend(step, own):
        zj = (z + step + NZ) % NZ
        kv = kvall[pl.ds(zj * NX, NX)].reshape(NX * S, CW)
        s = lax.dot_general(qbig[...], kv, (((1,), (1,)), ((), ())), preferred_element_type=F32)
        if own:
            row = lax.broadcasted_iota(jnp.int32, (2 * S, NX * S), 0)
            row = jnp.where(row >= S, row - S, row) + x * S
            col = lax.broadcasted_iota(jnp.int32, (2 * S, NX * S), 1)
            s = jnp.where(col <= row, s, MASKED)
        m_old = m_s[:, 0:1]
        m_new = jnp.maximum(m_old, jnp.max(s, axis=1, keepdims=True))
        alpha = jnp.exp2((m_old - m_new) * scale2)
        p = jnp.exp2((s - m_new) * scale2)
        l_new = l_s[:, 0:1] * alpha + jnp.sum(p, axis=1, keepdims=True)
        pv = jnp.dot(p.astype(BF), kv, preferred_element_type=F32)
        acc[...] = acc[...] * alpha + pv
        m_s[...] = jnp.broadcast_to(m_new, (2 * S, CW))
        l_s[...] = jnp.broadcast_to(l_new, (2 * S, CW))

    def attend_group(n):
        if steps[n] == 0:
            attend(0, True)
        else:

            @pl.when((z + steps[n] + NZ) % NZ < z)
            def _():
                attend(steps[n], False)

    z_up(0).start()
    z_dn(0).start()
    x_send(0)

    lanes = lax.broadcasted_iota(jnp.int32, (S, CW), 1)
    id0, id1 = ids_ref[:, 0:1], ids_ref[:, 1:2]
    oh0 = jnp.where(lanes == id0, 1.0, 0.0).astype(F32)
    oh1 = jnp.where(lanes == id1, 1.0, 0.0).astype(F32)
    low = jnp.where(
        lax.broadcasted_iota(jnp.int32, (S, S), 1) < lax.broadcasted_iota(jnp.int32, (S, S), 0),
        1.0, 0.0,
    ).astype(BF)
    cum = jnp.dot(low, (oh0 + oh1).astype(BF), preferred_element_type=F32)
    slots = lax.broadcasted_iota(jnp.int32, (S, ROWS), 1).astype(F32)
    for ident, oh, m in ((id0, oh0, m0), (id1, oh1, m1)):
        at = ident.astype(F32) * SLOT + jnp.sum(oh * cum, axis=1, keepdims=True)
        m[...] = jnp.where(slots == at, 1.0, 0.0).astype(BF)

    groups = [[0]]
    for k in range(4):
        groups.append([2 * k + 1] + ([2 * k + 2] if k < 3 else []))
    for k in range(4):
        got = kvall.at[slot(-1 - k)]
        rcopy(got, got, asend.at[0], zup.at[k], zdev(1)).wait_recv()
        if k < 3:
            z_up(k + 1).start()
        x_send(2 * k + 1)
        if k < 3:
            got = kvall.at[slot(1 + k)]
            rcopy(got, got, asend.at[0], zdn.at[k], zdev(-1)).wait_recv()
            if k < 2:
                z_dn(k + 1).start()
            x_send(2 * k + 2)
        for n in groups[k]:
            x_relay(n)
        if k >= 1:
            for n in groups[k - 1]:
                x_finish(n)
                attend_group(n)
    for n in groups[4]:
        x_relay(n)
    for g in (3, 4):
        for n in groups[g]:
            x_finish(n)
            attend_group(n)

    summed = acc[...] / l_s[...]
    diff = summed[0:S] - mw_ref[0] * summed[S:]
    lane = lax.broadcasted_iota(jnp.int32, (S, CW), 1)
    squares = jnp.sum(jnp.where(lane >= 64, diff * diff, 0.0), axis=1, keepdims=True) * (1.0 / 64)
    gain = hg_ref[...]
    head_out = (diff * lax.rsqrt(squares + EPS))[:, 64:] * gain
    hb[tp] = jnp.concatenate([head_out[0:HS], head_out[HS:]], axis=1).astype(BF)

    def direct_gather(buf, send, ring, pair):
        mine = buf.at[tp]
        for i in range(1, NY):
            rcopy(mine, mine, send.at[0], ring.at[i], ydev(i)).start()
        rcopy(mine, mine, send.at[0], pair.at[0], pair_dev).start()

    def direct_finish(buf, send, ring, pair):
        for i in (1, 7, 2, 6, 3, 5, 4):
            got = buf.at[(y - i + NY) % NY * 2 + c]
            rcopy(got, got, send.at[0], ring.at[i], ydev(i)).wait_recv()
            rcopy(got, got, send.at[0], pair.at[0], pair_dev).start()
        wait_bytes(buf.at[0:NY], pair.at[0])

    direct_gather(hb, bsend, bring, bpair)
    direct_finish(hb, bsend, bring, bpair)

    loads[0].wait()
    for j in range(NY):
        a, b = hb[2 * j], hb[2 * j + 1]
        hfull[0:HS, 128 * j : 128 * j + 128] = jnp.concatenate([a[:, :64], b[:, :64]], axis=1)
        hfull[HS:, 128 * j : 128 * j + 128] = jnp.concatenate([a[:, 64:], b[:, 64:]], axis=1)
    attn = jnp.dot(hfull[...], wo[...], preferred_element_type=F32)
    hidden = (res_ref[...].astype(F32) + attn).astype(BF)
    hid[...] = hidden
    own_cols = pl.ds(pl.multiple_of(tp * CW, CW), CW)
    hidall[:, own_cols] = hidden

    def ring_gather(view, total, parts, send, up, dn, pair, ready=None):
        def one(t, p, sem, dev):
            r = view(t, p)
            return rcopy(r, r, send.at[0], sem, dev)

        for p in range(parts):
            if ready is not None:
                ready(p)
            one(tp, p, up.at[p], ydev(1)).start()
            one(tp, p, dn.at[p], ydev(-1)).start()
            one(tp, p, pair.at[0], pair_dev).start()
        for k in range(4):
            for p in range(parts):
                for going_up in (True, False):
                    first = p < parts // 2
                    if k == 3 and first != going_up:
                        continue
                    step, sem = (1, up) if going_up else (-1, dn)
                    t = (y - step * (1 + k) + NY) % NY * 2 + c
                    one(t, p, sem.at[k * parts + p], ydev(step)).wait_recv()
                    if k < 2 or (k == 2 and first == going_up):
                        one(t, p, sem.at[(k + 1) * parts + p], ydev(step)).start()
                    one(t, p, pair.at[0], pair_dev).start()
        wait_bytes(total, pair.at[0])

    def c_view(t, p):
        rows = S // CP
        return hidall.at[p * rows : (p + 1) * rows, pl.ds(pl.multiple_of(t * CW, CW), CW)]

    ring_gather(c_view, hidall.at[:, 0:1024], CP, csend, cup, cdn, cpair)

    for r in range(2):
        full = hidall[r * HS : (r + 1) * HS, :].astype(F32)
        sq = jnp.mean(full * full, axis=1, keepdims=True)
        normed[r * HS : (r + 1) * HS, :] = (full * lax.rsqrt(sq + EPS) * ng_ref[...]).astype(BF)

    both = m0[...] + m1[...]
    picked = lax.dot_general(
        both, normed[:, own_cols], (((0,), (0,)), ((), ())), preferred_element_type=F32
    ).astype(BF)
    outg[...] = picked.reshape(NSP, SLOT, CW)
    own_rows = pl.ds(pl.multiple_of(sp * SLOT, SLOT), SLOT)
    eb_own = eb.at[own_rows, own_cols]
    eb_own[...] = outg[sp]

    def send_block(i, carry):
        e = (sp + i) % NSP
        rcopy(outg.at[e], eb.at[own_rows, own_cols], dsend.at[0], drecv.at[z // 2], (e, tp)).start()
        return carry

    lax.fori_loop(1, NSP, send_block, 0)

    def gated(gu):
        g = gu[:, 0:64]
        u = gu[:, 64:128]
        return g / (1.0 + jnp.exp(-g)) * u

    loads[4].wait()
    loads[5].wait()
    gu = lax.dot_general(
        normed[...], sgu[...], (((1,), (1,)), ((), ())), preferred_element_type=F32
    )
    h = gated(gu)
    sb[tp] = jnp.concatenate([h[0:HS], h[HS:]], axis=1).astype(BF)
    direct_gather(sb, ssend, sring, spair)

    prow = ROWS // EP

    def e_view(t, p):
        return eb.at[p * prow : (p + 1) * prow, pl.ds(pl.multiple_of(t * CW, CW), CW)]

    def e_ready(p):
        n = prow // SLOT

        @pl.when(z // 2 == p)
        def _():
            wait_bytes(outg.at[0 : n - 1], drecv.at[p])

        @pl.when(z // 2 != p)
        def _():
            wait_bytes(outg.at[0:n], drecv.at[p])

    ring_gather(e_view, eb.at[:, 0:1024], EP, esend, eup, edn, epair, e_ready)

    loads[1].wait()
    loads[2].wait()
    for r in range(2):
        lo, hi = [
            gated(
                lax.dot_general(
                    eb[r * 128 + o : r * 128 + o + 128, :], wgu[...],
                    (((1,), (1,)), ((), ())), preferred_element_type=F32,
                )
            )
            for o in (0, 256)
        ]
        fb[tp, r * 128 : (r + 1) * 128, :] = jnp.concatenate([lo, hi], axis=1).astype(BF)

    def f_view(t, p):
        rows = 256 // FP
        return fb.at[t, p * rows : (p + 1) * rows]

    ring_gather(f_view, fb.at[0:NY], FP, fsend, fup, fdn, fpair)

    loads[3].wait()
    for j in range(NY):
        a, b = fb[2 * j], fb[2 * j + 1]
        hidx[0:256, 128 * j : 128 * j + 128] = jnp.concatenate([a[:, :64], b[:, :64]], axis=1)
        hidx[256:, 128 * j : 128 * j + 128] = jnp.concatenate([a[:, 64:], b[:, 64:]], axis=1)
    for r in range(2):
        res = jnp.dot(hidx[r * 256 : (r + 1) * 256, :], wd[...], preferred_element_type=F32)
        res_o[r * 16 : (r + 1) * 16] = res.astype(BF).reshape(16, SLOT, CW)

    ret[sp] = res_o[sp]

    def return_block(i, carry):
        e = (sp + i) % NSP
        rcopy(res_o.at[e], ret.at[sp], gsend.at[0], grecv.at[0], (e, tp)).start()
        return carry

    lax.fori_loop(1, NSP, return_block, 0)

    direct_finish(sb, ssend, sring, spair)
    loads[6].wait()
    for j in range(NY):
        a, b = sb[2 * j], sb[2 * j + 1]
        hfull[0:HS, 128 * j : 128 * j + 128] = jnp.concatenate([a[:, :64], b[:, :64]], axis=1)
        hfull[HS:, 128 * j : 128 * j + 128] = jnp.concatenate([a[:, 64:], b[:, 64:]], axis=1)
    shared = jnp.dot(hfull[...], sd[...], preferred_element_type=F32)
    base = hid[...].astype(F32) + shared

    wait_bytes(outg.at[0 : NSP - 1], grecv.at[0])
    back = ret[...].reshape(ROWS, CW)
    r0 = jnp.dot(m0[...], back, preferred_element_type=F32)
    r1 = jnp.dot(m1[...], back, preferred_element_type=F32)
    routed = r0 * rw_ref[:, 0:1] + r1 * rw_ref[:, 1:2]
    out_ref[...] = (base + routed).astype(BF)

    wait_bytes(kvall.at[0 : NSP - 1], asend.at[0])
    wait_bytes(hb.at[0 : NT - 1], bsend.at[0])
    wait_bytes(hidall.at[:, 0 : 15 * CW], csend.at[0])
    wait_bytes(sb.at[0 : NT - 1], ssend.at[0])
    wait_bytes(outg.at[0 : NSP - 1], dsend.at[0])
    wait_bytes(eb.at[:, 0 : 15 * CW], esend.at[0])
    wait_bytes(fb.at[0 : NT - 1], fsend.at[0])
    wait_bytes(outg.at[0 : NSP - 1], gsend.at[0])


def body(
    residual_in, query_rows, key_rows, value_rows, map_weight, head_gain, out_proj, norm_gain,
    route_ids, route_weights, expert_gate, expert_up, expert_down, shared_gate, shared_up,
    shared_down,
):
    vm = pl.BlockSpec(memory_space=pltpu.VMEM)
    sm = pl.BlockSpec(memory_space=pltpu.SMEM)
    anyw = pl.BlockSpec(memory_space=pl.ANY)
    dma = pltpu.SemaphoreType.DMA
    v = pltpu.VMEM
    return pl.pallas_call(
        kernel,
        name="layer",
        out_shape=jax.ShapeDtypeStruct((S, CW), BF),
        in_specs=[vm, vm, vm, vm, sm, vm, vm, vm, vm] + [anyw] * 7,
        out_specs=vm,
        scratch_shapes=[
            v((NSP, S, CW), BF),
            v((2 * S, CW), BF),
            v((2 * S, CW), F32),
            v((2 * S, CW), F32),
            v((2 * S, CW), F32),
            v((1024, CW), BF),
            v((128, D), BF),
            v((1024, CW), BF),
            v((128, D), BF),
            v((1024, CW), BF),
            v((S, ROWS), BF),
            v((S, ROWS), BF),
            v((NT, HS, CW), BF),
            v((S, 1024), BF),
            v((S, CW), BF),
            v((S, D), BF),
            v((S, D), BF),
            v((NT, HS, CW), BF),
            v((NSP, SLOT, CW), BF),
            v((ROWS, D), BF),
            v((NT, 256, CW), BF),
            v((ROWS, 1024), BF),
            v((NSP, SLOT, CW), BF),
            v((NSP, SLOT, CW), BF),
            dma((7,)),
            dma((1,)), dma((4,)), dma((3,)), dma((8, 4)),
            dma((1,)), dma((8,)), dma((1,)),
            dma((1,)), dma((4 * CP,)), dma((4 * CP,)), dma((1,)),
            dma((1,)), dma((8,)), dma((1,)),
            dma((1,)), dma((EP,)),
            dma((1,)), dma((4 * EP,)), dma((4 * EP,)), dma((1,)),
            dma((1,)), dma((4 * FP,)), dma((4 * FP,)), dma((1,)),
            dma((1,)), dma((1,)),
        ],
        compiler_params=pltpu.CompilerParams(
            collective_id=0, has_side_effects=True, vmem_limit_bytes=60 * 1024 * 1024
        ),
    )(
        residual_in, query_rows, key_rows, value_rows, map_weight,
        head_gain.reshape(1, 64), norm_gain.reshape(1, D), route_ids, route_weights,
        out_proj, expert_gate, expert_up, expert_down, shared_gate, shared_up, shared_down,
    )


def solution(mesh):
    in_specs = (
        P("sp", "tp"),
        P("sp", "tp"),
        P("sp", "tp"),
        P("sp", "tp"),
        P("tp"),
        P(),
        P(None, "tp"),
        P(),
        P("sp", None),
        P("sp", None),
        P("sp", "tp", None),
        P("sp", "tp", None),
        P("sp", None, "tp"),
        P("tp", None),
        P("tp", None),
        P(None, "tp"),
    )
    return jax.shard_map(
        body, mesh=mesh, in_specs=in_specs, out_specs=P("sp", "tp"), check_vma=False
    )
```
